32 devices in a mesh: ep: 32 (over z, y, x, core).
Axes of the slice: x: 2, y: 2, z: 4, core: 2. Of those that a mesh axis runs over, the one named last changes fastest.
Arguments:
- tokens: bfloat16 [128, 2048], P('ep'), may hold values from -6 to 6
- recurrent_state: float32 [128, 8, 128, 128], P('ep'), may hold values from -4 to 4
- query_weight: bfloat16 [2048, 1024], P(None, 'ep'), may hold values from -0.125 to 0.125
- forget_weight: bfloat16 [2048, 1024], P(None, 'ep'), may hold values from -0.125 to 0.125
- input_weight: bfloat16 [2048, 1024], P(None, 'ep'), may hold values from -0.125 to 0.125
- outgate_weight: bfloat16 [2048, 1024], P(None, 'ep'), may hold values from -0.125 to 0.125
- lower_bound: float32 [1024], replicated, may hold values from 0 to 0.9
- head_gain: float32 [128], replicated, may hold values from 0.1 to 1.9
- mixout_weight: bfloat16 [1024, 2048], P(None, 'ep'), may hold values from -0.1875 to 0.1875
- first_gain: float32 [2048], replicated, may hold values from 0.1 to 1.9
- first_bias: float32 [2048], replicated, may hold values from -1.5 to 1.5
- router_weight: bfloat16 [2048, 8], replicated, may hold values from -0.125 to 0.125
- branch_vector: bfloat16 [2048], replicated, may hold values from -0.125 to 0.125
- dense_gate_weight: bfloat16 [2048, 5632], P(None, 'ep'), may hold values from -0.125 to 0.125
- dense_up_weight: bfloat16 [2048, 5632], P(None, 'ep'), may hold values from -0.125 to 0.125
- dense_down_weight: bfloat16 [5632, 2048], P('ep'), may hold values from -0.078125 to 0.078125
- expert_gate_weight: bfloat16 [2048, 57344], P(None, 'ep'), may hold values from -0.125 to 0.125
- expert_up_weight: bfloat16 [2048, 57344], P(None, 'ep'), may hold values from -0.125 to 0.125
- expert_down_weight: bfloat16 [57344, 2048], P('ep'), may hold values from -0.0625 to 0.0625
- second_gain: float32 [2048], replicated, may hold values from 0.1 to 1.9
- second_bias: float32 [2048], replicated, may hold values from -1.5 to 1.5
- routes: int32 [128, 2], replicated, may hold values from 0 to 7, all different within a row; in each aligned block of 4 rows (0 to 3, 4 to 7, ...) at most 2 rows name the same one
Outputs:
- output: bfloat16 [128, 2048], P('ep')
- new_state: float32 [128, 8, 128, 128], P('ep')
The draws below stay inside these ranges and needn't reach their ends.
Inputs may be any that keep to these rules, and one draw needn't show every extreme that they name: `routes`: each row names two different experts; in the rows of one device no expert is named more than 2 times, a bound that some block reaches in some device's rows.
All inputs are finite; a program needn't handle non-finite values.
Results may differ from the reference program's by a relative error of at most 0.0095.
Values may be sent and summed in bfloat16 or wider, within the bound.
A program may use at most 64 MiB of HBM per device.

```python
import math
import jax
import jax.numpy as jnp
import numpy as np
from jax import lax

D = 2048
HGW = 1024
DK = 128
HEADS = 8
EXPERTS = 8
FF_E = 7168
FD = 5632
B_DEV = 4
CAP = 2
TOKENS = 128
N_EP = 32


def block_scale(rng, extent, cuts, least, high):
    level, own = 1.0, jax.random.fold_in(rng, 6)
    for axis_at, blocks in cuts:
        draws = jnp.exp(jax.random.uniform(jax.random.fold_in(own, axis_at), (blocks,), jnp.float32, least / len(cuts), high / len(cuts)))
        level = level * jnp.repeat(draws, extent[axis_at] // blocks).reshape([-1 if axis == axis_at else 1 for axis in range(len(extent))])
    return level


def deal_out(key, own, number, rows, amount, top, reach, skew):
    order = jax.random.permutation(key, amount)
    crowded, usual = portions_of(amount, rows * top, reach, skew, True), portions_of(amount, rows * top, reach, skew, False)
    places = jnp.arange(amount)

    def named(sizes, rotation):
        used = int((sizes > 0).sum())
        fixed = max(1, used // 4)
        moved = fixed + (places - fixed + rotation * (used - fixed)) % max(1, amount - fixed)
        return jnp.zeros((amount,), jnp.int32).at[order[jnp.where(places < fixed, places, moved)]].set(jnp.asarray(sizes, jnp.int32))

    sizes = jnp.where(number % 4 == 0, named(crowded, number // 4), named(usual, number - number // 4 - 1))
    mixed = jax.random.permutation(jax.random.fold_in(own, 3), amount)
    donor, sink = mixed[0:amount // 2 * 2:2], mixed[1:amount // 2 * 2:2]
    room = jnp.minimum(sizes[donor] - 1, reach - sizes[sink]) // 2
    room = jnp.where((donor == order[0]) | (sink == order[0]) | (sizes[sink] == 0), 0, jnp.maximum(room, 0))
    moved = jax.random.randint(jax.random.fold_in(own, 4), (amount // 2,), 0, 1 << 20) % (room + 1)
    sizes = sizes.at[donor].add(-moved).at[sink].add(moved)
    members = jnp.searchsorted(jnp.cumsum(sizes), jnp.arange(rows * top), side="right").astype(jnp.int32)
    table = members.reshape(top, rows).T
    table = table[jax.random.permutation(jax.random.fold_in(own, 1), rows)]
    rotation = jax.random.randint(jax.random.fold_in(own, 2), (rows, 1), 0, top)
    return jnp.take_along_axis(table, (jnp.arange(top)[None, :] + rotation) % top, axis=1)


def portions_of(amount, total, reach, slope, full):
    weights = [(1 << 20) // math.isqrt(rank ** slope) + 1 for rank in range(1, amount + 1)]
    largest = reach if full else min(reach, max(-(-total // amount), total * weights[0] // sum(weights)))
    least = 1 if total - largest >= amount - 1 else 0
    holding, spare = [largest] + [least] * (amount - 1), total - largest - least * (amount - 1)
    while spare > 0:
        free = [i for i in range(1, amount) if holding[i] < largest] or [i for i in range(1, amount) if holding[i] < reach]
        mass, remaining = sum([weights[i] for i in free]), spare
        for i in free:
            addition = min(reach - holding[i], max(1, remaining * weights[i] // mass), spare)
            holding[i] = holding[i] + addition
            spare = spare - addition
    return np.array(holding)


def bell_draw(stream_key, shape, scale, limit, pieces=(), kind=jnp.bfloat16):
    level = block_scale(stream_key, shape, pieces, -0.22, 0.18) if pieces else 1.0
    result = jax.random.normal(stream_key, shape, jnp.float32) * scale * level
    return jnp.minimum(jnp.maximum(result, -limit), limit).astype(kind)


def setup_inputs(seed: int = 0) -> dict:
    keys = jax.random.split(jax.random.key(seed), 23)
    tokens = bell_draw(keys[0], (TOKENS, D), 1.0, 6.0, ((0, 32),))
    recurrent_state = bell_draw(keys[1], (TOKENS, HEADS, DK, DK), 0.5, 4.0, ((0, 32),), jnp.float32)
    query_weight = bell_draw(keys[2], (D, HGW), D ** -0.5, 0.125, ((1, 32),))
    forget_weight = bell_draw(keys[3], (D, HGW), D ** -0.5, 0.125, ((1, 32),))
    input_weight = bell_draw(keys[4], (D, HGW), D ** -0.5, 0.125, ((1, 32),))
    outgate_weight = bell_draw(keys[5], (D, HGW), D ** -0.5, 0.125, ((1, 32),))
    lower_bound = jnp.clip(jax.random.uniform(keys[6], (HGW,), jnp.float32, 0.0, 0.9), 0.0, 0.9)
    head_gain = jnp.clip(1.0 + 0.18 * jax.random.normal(keys[7], (DK,), jnp.float32), 0.1, 1.9)
    mixout_weight = bell_draw(keys[8], (HGW, D), HGW ** -0.5, 0.1875, ((1, 32),))
    first_gain = jnp.clip(1.0 + 0.18 * jax.random.normal(keys[9], (D,), jnp.float32), 0.1, 1.9)
    first_bias = bell_draw(keys[10], (D,), 0.3, 1.5, (), jnp.float32)
    router_weight = bell_draw(keys[11], (D, EXPERTS), D ** -0.5, 0.125)
    branch_vector = bell_draw(keys[12], (D,), D ** -0.5, 0.125)
    dense_gate_weight = bell_draw(keys[13], (D, FD), D ** -0.5, 0.125, ((1, 32),))
    dense_up_weight = bell_draw(keys[14], (D, FD), D ** -0.5, 0.125, ((1, 32),))
    dense_down_weight = bell_draw(keys[15], (FD, D), FD ** -0.5, 0.078125, ((0, 32),))
    expert_gate_weight = bell_draw(keys[16], (D, EXPERTS * FF_E), D ** -0.5, 0.125, ((1, 32),))
    expert_up_weight = bell_draw(keys[17], (D, EXPERTS * FF_E), D ** -0.5, 0.125, ((1, 32),))
    expert_down_weight = bell_draw(keys[18], (EXPERTS * FF_E, D), FF_E ** -0.5, 0.0625, ((0, 32),))
    second_gain = jnp.clip(1.0 + 0.18 * jax.random.normal(keys[19], (D,), jnp.float32), 0.1, 1.9)
    second_bias = bell_draw(keys[20], (D,), 0.3, 1.5, (), jnp.float32)
    routes_keys = jax.random.split(jax.random.fold_in(keys[21], 1), TOKENS // B_DEV)
    routes_turns = jax.random.permutation(jax.random.fold_in(keys[21], 3), TOKENS // B_DEV)
    routes = jax.vmap(lambda own, number: deal_out(jax.random.fold_in(keys[21], 2), own, number, B_DEV, EXPERTS, 2, CAP, 2))(routes_keys, routes_turns).reshape((TOKENS, 2))
    return dict(tokens=tokens, recurrent_state=recurrent_state, query_weight=query_weight, forget_weight=forget_weight, input_weight=input_weight, outgate_weight=outgate_weight, lower_bound=lower_bound, head_gain=head_gain, mixout_weight=mixout_weight, first_gain=first_gain, first_bias=first_bias, router_weight=router_weight, branch_vector=branch_vector, dense_gate_weight=dense_gate_weight, dense_up_weight=dense_up_weight, dense_down_weight=dense_down_weight, expert_gate_weight=expert_gate_weight, expert_up_weight=expert_up_weight, expert_down_weight=expert_down_weight, second_gain=second_gain, second_bias=second_bias, routes=routes)


ALPHA = 8.0 ** 0.25
NORM_EPS = 1e-05
HEAD_EPS = 1e-06

def layer_norm(mixture, gain, bias):
    center = lax.optimization_barrier(jnp.mean(mixture, axis=-1, keepdims=True))
    spread = lax.optimization_barrier(jnp.mean(jnp.square(mixture - center), axis=-1, keepdims=True))
    return (mixture - center) * lax.rsqrt(spread + NORM_EPS) * gain + bias

def recurrence(projected, state, lower_bound, head_gain):
    nseq, heads, width = (state.shape[0], state.shape[1], state.shape[2])
    query = projected[:, 0].astype(jnp.float32).reshape(nseq, heads, width)
    forget_in = projected[:, 1].astype(jnp.float32)
    value = projected[:, 2].astype(jnp.float32).reshape(nseq, heads, width)
    outgate = projected[:, 3].astype(jnp.float32)
    forget = (lower_bound + (1.0 - lower_bound) * jax.nn.sigmoid(forget_in)).reshape(nseq, heads, width)
    keyed = ((1.0 - lower_bound) * jax.nn.sigmoid(-forget_in)).reshape(nseq, heads, width)
    fresh = forget[..., None] * state + keyed[..., None] * value[:, :, None, :]
    read = jnp.einsum('bhkv,bhk->bhv', fresh, query, precision=lax.Precision.HIGHEST)
    scaled = read * lax.rsqrt(lax.optimization_barrier(jnp.mean(jnp.square(read), axis=-1, keepdims=True)) + HEAD_EPS) * head_gain
    mixed = (scaled.reshape(nseq, heads * width) * jax.nn.silu(outgate)).astype(jnp.bfloat16)
    return (mixed, fresh)

def reference(tokens, recurrent_state, query_weight, forget_weight, input_weight, outgate_weight, lower_bound, head_gain, mixout_weight, first_gain, first_bias, router_weight, branch_vector, dense_gate_weight, dense_up_weight, dense_down_weight, expert_gate_weight, expert_up_weight, expert_down_weight, second_gain, second_bias, routes):
    f32 = jnp.float32
    parts = [jnp.dot(tokens, weight, preferred_element_type=f32).astype(jnp.bfloat16) for weight in (query_weight, forget_weight, input_weight, outgate_weight)]
    projected = jnp.stack(parts, axis=1)
    mixed, new_state = recurrence(projected, recurrent_state, lower_bound, head_gain)
    mix_out = jnp.dot(mixed, mixout_weight, preferred_element_type=f32).astype(jnp.bfloat16)
    normed = layer_norm(ALPHA * tokens.astype(f32) + mix_out.astype(f32), first_gain, first_bias).astype(jnp.bfloat16)
    width = normed.shape[1]
    logits = jnp.dot(normed, router_weight, preferred_element_type=f32)
    expert_ids = jnp.arange(EXPERTS, dtype=jnp.int32)
    first_pick = routes[:, 0]
    second_pick = routes[:, 1]
    first_logit = lax.optimization_barrier(jnp.sum(jnp.where(first_pick[:, None] == expert_ids[None, :], logits, 0.0), axis=1))
    second_logit = lax.optimization_barrier(jnp.sum(jnp.where(second_pick[:, None] == expert_ids[None, :], logits, 0.0), axis=1))
    share = jax.nn.sigmoid(first_logit - second_logit)
    branch_gate = jax.nn.sigmoid(jnp.dot(normed, branch_vector, preferred_element_type=f32))
    dense_hidden = (jax.nn.silu(jnp.dot(normed, dense_gate_weight, preferred_element_type=f32)) * jnp.dot(normed, dense_up_weight, preferred_element_type=f32)).astype(jnp.bfloat16)
    channel = branch_gate[:, None] * jnp.dot(dense_hidden, dense_down_weight, preferred_element_type=f32)
    blocks = normed.reshape(N_EP, B_DEV, width).astype(f32)
    slot_ids = jnp.arange(CAP, dtype=jnp.int32)
    for expert in range(EXPERTS):
        on_first = first_pick == expert
        on_second = second_pick == expert
        token_weight = share * on_first.astype(f32) + (1.0 - share) * on_second.astype(f32)
        hits = (on_first | on_second).astype(jnp.int32).reshape(N_EP, B_DEV)
        ranks = jnp.cumsum(hits, axis=1) - 1
        select = ((ranks[:, None, :] == slot_ids[None, :, None]) & (hits[:, None, :] > 0)).astype(f32)
        slot_rows = jnp.einsum('sci,sid->scd', select, blocks, precision=lax.Precision.HIGHEST)
        slot_rows = slot_rows.astype(jnp.bfloat16).reshape(N_EP * CAP, width)
        low = expert * FF_E
        gate_part = jnp.dot(slot_rows, expert_gate_weight[:, low:low + FF_E], preferred_element_type=f32)
        up_part = jnp.dot(slot_rows, expert_up_weight[:, low:low + FF_E], preferred_element_type=f32)
        hidden = (jax.nn.silu(gate_part) * up_part).astype(jnp.bfloat16)
        slot_out = jnp.dot(hidden, expert_down_weight[low:low + FF_E, :], preferred_element_type=f32)
        slot_out = slot_out.reshape(N_EP, CAP, width)
        back = jnp.einsum('sci,scd->sid', select, slot_out, precision=lax.Precision.HIGHEST)
        channel = channel + back.reshape(N_EP * B_DEV, width) * token_weight[:, None]
    output = layer_norm(ALPHA * normed.astype(f32) + channel, second_gain, second_bias).astype(jnp.bfloat16)
    return (output, new_state)
```

```python
import jax
import jax.numpy as jnp
from jax import lax
import functools

from jax.experimental import pallas as pl
from jax.experimental.pallas import tpu as pltpu
from jax.sharding import PartitionSpec as P

EXPERTS = 8
CHUNKS = 4
MESH = pl.DeviceIdType.MESH


ALPHA = 8.0**0.25
NORM_EPS = 1e-05
HEAD_EPS = 1e-06


def layer_norm(mixture, gain, bias):
    center = jnp.mean(mixture, axis=-1, keepdims=True)
    spread = jnp.mean(jnp.square(mixture - center), axis=-1, keepdims=True)
    return (mixture - center) * lax.rsqrt(spread + NORM_EPS) * gain + bias


def recurrence(projected, state, lower_bound, head_gain):
    nseq, heads, width = (state.shape[0], state.shape[1], state.shape[2])
    query = projected[:, 0].astype(jnp.float32).reshape(nseq, heads, width)
    forget_in = projected[:, 1].astype(jnp.float32)
    value = projected[:, 2].astype(jnp.float32).reshape(nseq, heads, width)
    outgate = projected[:, 3].astype(jnp.float32)
    forget = (lower_bound + (1.0 - lower_bound) * jax.nn.sigmoid(forget_in)).reshape(
        nseq, heads, width
    )
    keyed = ((1.0 - lower_bound) * jax.nn.sigmoid(-forget_in)).reshape(nseq, heads, width)
    fresh = forget[..., None] * state + keyed[..., None] * value[:, :, None, :]
    read = jnp.einsum("bhkv,bhk->bhv", fresh, query, precision=lax.Precision.HIGHEST)
    scaled = (
        read * lax.rsqrt(jnp.mean(jnp.square(read), axis=-1, keepdims=True) + HEAD_EPS) * head_gain
    )
    mixed = (scaled.reshape(nseq, heads * width) * jax.nn.silu(outgate)).astype(jnp.bfloat16)
    return (mixed, fresh)


def greet(n, me):
    barrier = pltpu.get_barrier_semaphore()

    @pl.loop(1, n)
    def _(k):
        pl.semaphore_signal(
            barrier, inc=1, device_id=(lax.rem(me + k, n),), device_id_type=MESH
        )

    pl.semaphore_wait(barrier, n - 1)


def start_all(source, dest, send_sem, recv_sem, n, me):
    @pl.loop(1, n)
    def _(k):
        peer = lax.rem(me + k, n)
        pltpu.make_async_remote_copy(
            src_ref=source(peer),
            dst_ref=dest.at[me],
            send_sem=send_sem.at[k],
            recv_sem=recv_sem.at[k],
            device_id=(peer,),
            device_id_type=MESH,
        ).start()


def wait_all(source, dest, send_sem, recv_sem, n, me):
    @pl.loop(1, n)
    def _(k):
        peer = lax.rem(me + k, n)
        pltpu.make_async_remote_copy(
            src_ref=source(peer),
            dst_ref=dest.at[lax.rem(me + n - k, n)],
            send_sem=send_sem.at[k],
            recv_sem=recv_sem.at[k],
            device_id=(peer,),
            device_id_type=MESH,
        ).wait()


def gather_all(block_ref, gathered, send_sem, recv_sem, n, me):
    chips = n // 2
    chip, core = lax.div(me, 2), lax.rem(me, 2)
    sibling = 2 * chip + 1 - core

    def across(k, owner):
        return pltpu.make_async_remote_copy(
            src_ref=block_ref,
            dst_ref=gathered.at[owner],
            send_sem=send_sem.at[k],
            recv_sem=recv_sem.at[k],
            device_id=(2 * lax.rem(chip + k, chips) + core,),
            device_id_type=MESH,
        )

    def onward(k, source, owner):
        return pltpu.make_async_remote_copy(
            src_ref=source,
            dst_ref=gathered.at[owner],
            send_sem=send_sem.at[chips + k],
            recv_sem=recv_sem.at[chips + k],
            device_id=(sibling,),
            device_id_type=MESH,
        )

    pl.loop(1, chips)(lambda k: across(k, me).start())
    onward(0, block_ref, me).start()
    gathered[me] = block_ref[...]

    @pl.loop(1, chips)
    def _(k):
        owner = 2 * lax.rem(chip + chips - k, chips) + core
        across(k, owner).wait()
        onward(k, gathered.at[owner], owner).start()

    onward(0, block_ref, sibling).wait()

    @pl.loop(1, chips)
    def _(k):
        base = 2 * lax.rem(chip + chips - k, chips)
        onward(k, gathered.at[base + core], base + 1 - core).wait()


def dot_turned(rows, weight):
    return lax.dot_general(
        rows, weight, (((1,), (1,)), ((), ())), preferred_element_type=jnp.float32
    )


def flatten_rows(blocks, flat, n, nseq):
    group = max(1, 16 // nseq)

    @pl.loop(0, n // group)
    def _(i):
        parts = [blocks[i * group + j].astype(jnp.float32) for j in range(group)]
        at = pl.multiple_of(i * (group * nseq), group * nseq)
        flat[pl.ds(at, group * nseq), :] = jnp.concatenate(parts, axis=0).astype(flat.dtype)


def split_rows(flat, blocks, n, nseq):
    group = max(1, 8 // nseq)

    @pl.loop(0, n // group)
    def _(i):
        at = pl.multiple_of(i * (group * nseq), group * nseq)
        taken = flat[pl.ds(at, group * nseq), :]
        for j in range(group):
            blocks[i * group + j] = taken[j * nseq : (j + 1) * nseq].astype(blocks.dtype)


def project_kernel(
    n, block_ref, weight_hbm, out_ref,
    weight, gathered, rows, made, outgoing, landed,
    weight_sem, gather_send, gather_recv, back_send, back_recv,
):
    me = lax.axis_index("ep")
    nseq = block_ref.shape[0]
    load = pltpu.make_async_copy(weight_hbm, weight, weight_sem)
    load.start()
    greet(n, me)
    gather_all(block_ref, gathered, gather_send, gather_recv, n, me)
    flatten_rows(gathered, rows, n, nseq)
    load.wait()
    made[...] = dot_turned(rows[...], weight[...])
    split_rows(made, outgoing, n, nseq)
    part = lambda peer: outgoing.at[peer]
    start_all(part, landed, back_send, back_recv, n, me)
    landed[me] = outgoing[me]
    wait_all(part, landed, back_send, back_recv, n, me)
    out_ref[...] = landed[...]


def exchange_semaphores(n):
    return [pltpu.SemaphoreType.DMA((n,))] * 4


def project(block, weight, n, collective_id):
    nseq, width = block.shape
    cols = weight.shape[0]
    bf16, f32 = jnp.bfloat16, jnp.float32
    return pl.pallas_call(
        functools.partial(project_kernel, n),
        out_shape=jax.ShapeDtypeStruct((n, nseq, cols), bf16),
        in_specs=[
            pl.BlockSpec(memory_space=pltpu.VMEM),
            pl.BlockSpec(memory_space=pl.ANY),
        ],
        out_specs=pl.BlockSpec(memory_space=pltpu.VMEM),
        scratch_shapes=[
            pltpu.VMEM(weight.shape, bf16),
            pltpu.VMEM((n, nseq, width), bf16),
            pltpu.VMEM((n * nseq, width), bf16),
            pltpu.VMEM((n * nseq, cols), f32),
            pltpu.VMEM((n, nseq, cols), bf16),
            pltpu.VMEM((n, nseq, cols), bf16),
            pltpu.SemaphoreType.DMA,
            *exchange_semaphores(n),
        ],
        compiler_params=pltpu.CompilerParams(
            collective_id=collective_id, has_side_effects=True, vmem_limit_bytes=24 * 2**20
        ),
    )(block, weight)


def column_tile(cols):
    return 256 if cols % 256 == 0 else cols


def for_tiles(cols, body):
    tile = column_tile(cols)
    if tile == cols:
        body(slice(None))
    else:
        pl.loop(0, cols // tile)(lambda i: body(pl.ds(pl.multiple_of(i * tile, tile), tile)))


def channel_kernel(
    n, block_ref, pick_ref, small_ref, gain_ref, bias_ref,
    gate_hbm, up_hbm, down_hbm, dense_gate_hbm, dense_up_hbm, dense_down_hbm, out_ref,
    gate_w, up_w, down_w, dense_gate_w, dense_up_w, dense_down_w,
    gathered, rows, hidden, dense_hidden, made, outgoing, landed,
    weight_sem, gather_send, gather_recv, back_send, back_recv,
):
    f32 = jnp.float32
    me = lax.axis_index("ep")
    nseq, width = block_ref.shape
    pairs = (
        (dense_gate_hbm, dense_gate_w),
        (dense_up_hbm, dense_up_w),
        (gate_hbm, gate_w),
        (up_hbm, up_w),
        (dense_down_hbm, dense_down_w),
        (down_hbm, down_w),
    )
    loads = [
        pltpu.make_async_copy(there, here, weight_sem.at[i]) for i, (there, here) in enumerate(pairs)
    ]
    for load in loads:
        load.start()
    greet(n, me)
    gather_all(block_ref, gathered, gather_send, gather_recv, n, me)
    flatten_rows(gathered, rows, n, nseq)
    dot = functools.partial(jnp.dot, preferred_element_type=f32)

    small = dot_turned(rows[...], small_ref[...])
    picks = pick_ref[...]
    logit_gap = jnp.sum(small[:, :EXPERTS] * picks[:, :EXPERTS], axis=1, keepdims=True)
    share = jax.nn.sigmoid(logit_gap)
    branch_gate = jax.nn.sigmoid(small[:, EXPERTS : EXPERTS + 1])
    on_first = picks[:, EXPERTS : EXPERTS + 1] > 0
    on_second = picks[:, EXPERTS + 1 : EXPERTS + 2] > 0
    weight = jnp.where(on_first, share, jnp.where(on_second, 1.0 - share, 0.0))

    def fill(target, gate, up):
        def body(at):
            gate_part = dot(rows[...], gate[:, at])
            up_part = dot(rows[...], up[:, at])
            target[:, at] = (jax.nn.silu(gate_part) * up_part).astype(jnp.bfloat16)

        for_tiles(target.shape[1], body)

    for load in loads[:2]:
        load.wait()
    gate_part = dot_turned(rows[...], dense_gate_w[...])
    up_part = dot_turned(rows[...], dense_up_w[...])
    dense_hidden[...] = (jax.nn.silu(gate_part) * up_part).astype(jnp.bfloat16)
    for load in loads[2:4]:
        load.wait()
    fill(hidden, gate_w, up_w)
    for load in loads[4:]:
        load.wait()

    def down(at):
        routed = dot(hidden[...], down_w[:, at])
        dense = dot(dense_hidden[...], dense_down_w[:, at])
        made[:, at] = branch_gate * dense + jnp.where(weight > 0, weight * routed, 0.0)

    for_tiles(width, down)
    split_rows(made, outgoing, n, nseq)
    part = lambda peer: outgoing.at[peer]
    start_all(part, landed, back_send, back_recv, n, me)
    landed[me] = outgoing[me]
    wait_all(part, landed, back_send, back_recv, n, me)
    channel = lax.fori_loop(
        0, n, lambda d, total: total + landed[d].astype(f32), jnp.zeros((nseq, width), f32)
    )
    mixture = ALPHA * block_ref[...].astype(f32) + channel
    out_ref[...] = layer_norm(mixture, gain_ref[...], bias_ref[...]).astype(jnp.bfloat16)


def channel_and_norm(
    normed, routes, n, router_weight, branch_vector, dense_gate_weight, dense_up_weight,
    dense_down_weight, expert_gate_weight, expert_up_weight, expert_down_weight, gain, bias,
):
    bf16, f32 = jnp.bfloat16, jnp.float32
    nseq, width = normed.shape
    total = n * nseq
    expert = lax.axis_index("ep") // (n // EXPERTS)
    first = jax.nn.one_hot(routes[:, 0], EXPERTS, dtype=f32)
    second = jax.nn.one_hot(routes[:, 1], EXPERTS, dtype=f32)
    picks = jnp.concatenate([first - second, (routes == expert).astype(f32)], axis=1)
    small = jnp.concatenate([router_weight.T, branch_vector[None]], axis=0)
    weights = (
        expert_gate_weight,
        expert_up_weight,
        expert_down_weight,
        dense_gate_weight.T,
        dense_up_weight.T,
        dense_down_weight,
    )
    vmem, anywhere = pl.BlockSpec(memory_space=pltpu.VMEM), pl.BlockSpec(memory_space=pl.ANY)
    return pl.pallas_call(
        functools.partial(channel_kernel, n),
        out_shape=jax.ShapeDtypeStruct((nseq, width), bf16),
        in_specs=[vmem] * 5 + [anywhere] * 6,
        out_specs=vmem,
        scratch_shapes=[
            *[pltpu.VMEM(w.shape, bf16) for w in weights],
            pltpu.VMEM((n, nseq, width), bf16),
            pltpu.VMEM((total, width), bf16),
            pltpu.VMEM((total, expert_gate_weight.shape[1]), bf16),
            pltpu.VMEM((total, dense_gate_weight.shape[1]), bf16),
            pltpu.VMEM((total, width), f32),
            pltpu.VMEM((n, nseq, width), bf16),
            pltpu.VMEM((n, nseq, width), bf16),
            pltpu.SemaphoreType.DMA((6,)),
            *exchange_semaphores(n),
        ],
        compiler_params=pltpu.CompilerParams(
            collective_id=2, has_side_effects=True, vmem_limit_bytes=56 * 2**20
        ),
    )(normed, picks, small, gain[None], bias[None], *weights)


def parity_peers(chip, chips):
    bits = [1 << i for i in range(chips.bit_length() - 1)]
    steps = [(1 - 2 * lax.rem(lax.div(chip, bit), 2)) * bit for bit in bits]
    peers = []
    for k in range(chips):
        peer = chip
        for bit, step in zip(bits, steps):
            if k & bit:
                peer = peer + step
        peers.append(peer)
    return peers


def remote(source, dest, send_sem, recv_sem, device):
    return pltpu.make_async_remote_copy(
        src_ref=source, dst_ref=dest, send_sem=send_sem, recv_sem=recv_sem,
        device_id=(device,), device_id_type=MESH,
    )


def stack_rows(blocks, flat, chips, nseq):
    group = 16 // nseq
    for i in range(chips // group):
        parts = [blocks[i * group + j].astype(jnp.float32) for j in range(group)]
        flat[i * 16 : (i + 1) * 16, :] = jnp.concatenate(parts, axis=0).astype(flat.dtype)


def layer_kernel(
    n, chunks,
    tokens_hbm, state_hbm, query_hbm, forget_hbm, value_hbm, outgate_hbm, bound_hbm, head_gain_hbm,
    mixout_hbm, first_gain_hbm, first_bias_hbm, router_hbm, branch_hbm,
    dense_gate_hbm, dense_up_hbm, dense_down_hbm, gate_hbm, up_hbm, down_hbm,
    second_gain_hbm, second_bias_hbm, routes_hbm,
    out_ref, fresh_ref,
    state, query_w, mix_w, gate_w, up_w, down_w, dense_gate_w, dense_up_w, dense_down_w,
    bound, head_gain, first_gain, first_bias, router, branch, second_gain, second_bias, routes,
    tok_blocks, tok_rows, made_out, made_in, mix_blocks, mix_rows, feats, normed,
    state_high, state_low, small_w, hidden, dense_hidden, own_part, pair_out, pair_in,
    outgoing, landed,
    load_sem, a_send, a_recv, b_send, b_recv, c_send, c_recv, d_send, d_recv, f_send, f_recv,
    pair_send, pair_recv,
):
    bf16, f32 = jnp.bfloat16, jnp.float32
    me = lax.axis_index("ep")
    chips = n // 2
    chip, core = lax.div(me, 2), lax.rem(me, 2)
    sibling = 2 * chip + 1 - core
    peers = parity_peers(chip, chips)
    devices = [2 * peer + core for peer in peers]
    order = list(range(chips - 1, 0, -1))
    nseq, width = tokens_hbm.shape
    heads, depth = bound.shape
    half = chips * nseq
    own = query_hbm.shape[0]
    mix_own = mixout_hbm.shape[0]
    at_core = lambda base, size: pl.ds(pl.multiple_of(base + core * size, size), size)

    loads = []

    def load(there, here):
        copy = pltpu.make_async_copy(there, here, load_sem.at[len(loads)])
        copy.start()
        loads.append(copy)
        return copy

    get_tokens = load(tokens_hbm, tok_blocks.at[chip])
    pieces = (query_hbm, forget_hbm, value_hbm, outgate_hbm)
    spots = [query_w.at[at_core(m * 2 * own, own)] for m in range(4)]
    get_proj = [load(piece, spot) for piece, spot in zip(pieces, spots)]
    mix_spot = mix_w.at[at_core(0, mix_own)]
    get_mix = load(mixout_hbm, mix_spot)
    get_small = [
        load(there, here)
        for there, here in (
            (bound_hbm, bound), (head_gain_hbm, head_gain), (first_gain_hbm, first_gain),
            (first_bias_hbm, first_bias), (router_hbm, router), (branch_hbm, branch),
            (second_gain_hbm, second_gain), (second_bias_hbm, second_bias), (routes_hbm, routes),
        )
    ]
    get_state = load(state_hbm, state)
    get_dense = [load(dense_gate_hbm, dense_gate_w), load(dense_up_hbm, dense_up_w)]
    get_wide = [load(gate_hbm, gate_w), load(up_hbm, up_w)]
    get_down = [load(dense_down_hbm, dense_down_w), load(down_hbm, down_w)]

    barrier = pltpu.get_barrier_semaphore()
    for k in order:
        pl.semaphore_signal(barrier, inc=1, device_id=(devices[k],), device_id_type=MESH)
    pl.semaphore_signal(barrier, inc=1, device_id=(sibling,), device_id_type=MESH)
    get_tokens.wait()
    for copy in get_proj:
        copy.wait()
    get_mix.wait()
    pl.semaphore_wait(barrier, chips)

    sent = []

    def spread(source, dest, send_sem, recv_sem):
        for k in order:
            copy = remote(source(k), dest.at[chip], send_sem.at[k], recv_sem.at[k], devices[k])
            copy.start()
            sent.append(copy)

    def arrive(source, dest, send_sem, recv_sem):
        for k in order:
            remote(
                source(k), dest.at[peers[k]], send_sem.at[k], recv_sem.at[k], devices[k]
            ).wait_recv()

    def swap(source, dest, i):
        copy = remote(source, dest, pair_send.at[i], pair_recv.at[i], sibling)
        copy.start()
        sent.append(copy)

    def swapped(source, dest, i):
        remote(source, dest, pair_send.at[i], pair_recv.at[i], sibling).wait_recv()

    own_tokens = lambda k: tok_blocks.at[chip]
    spread(own_tokens, tok_blocks, a_send, a_recv)
    for m in range(4):
        swap(spots[m], spots[m], m)
    swap(mix_spot, mix_spot, 4)

    for copy in get_small:
        copy.wait()
    spread_rows = lambda rows: jnp.concatenate(
        [jnp.broadcast_to(rows[h : h + 1], (nseq, depth)) for h in range(heads)], axis=0
    )
    bounds = spread_rows(bound[...])
    branch_row = jnp.concatenate([branch[i : i + 1, :].astype(f32) for i in range(branch.shape[0])], axis=1)
    small_w[...] = jnp.concatenate(
        [router[...].astype(f32), branch_row, jnp.zeros((16 - EXPERTS - 1, width), f32)], axis=0
    ).astype(bf16)

    total = n * nseq
    expert = lax.div(me, n // EXPERTS)
    first, second = routes[0:1, :], routes[1:2, :]
    ids = lax.broadcasted_iota(jnp.int32, (EXPERTS, total), 0)
    gap = (first == ids).astype(f32) - (second == ids).astype(f32)
    table = jnp.concatenate(
        [gap, (first == expert).astype(f32), (second == expert).astype(f32),
         jnp.zeros((16 - EXPERTS - 2, total), f32)], axis=0,
    ).astype(bf16)
    row = lax.broadcasted_iota(jnp.int32, (total, total), 0)
    column = lax.broadcasted_iota(jnp.int32, (total, total), 1)
    local = jnp.where(row < half, row, row - half)
    parity = jnp.where(row < half, core, 1 - core)
    which = (2 * (local // nseq) + parity) * nseq + local % nseq
    turn = (which == column).astype(f32).astype(bf16)
    picks = dot_turned(turn, table)

    get_state.wait()
    for p in range(heads // 2):
        for q in range(nseq // 2):
            for a in range(2):
                for b in range(2):
                    block = state[(2 * q + b) * heads + 2 * p + a]
                    high = block.astype(bf16)
                    low = (block - high.astype(f32)).astype(bf16)
                    at = (p * (nseq // 2) + q, slice(a * depth, (a + 1) * depth), slice(b * depth, (b + 1) * depth))
                    state_high[at] = high
                    state_low[at] = low

    arrive(own_tokens, tok_blocks, a_send, a_recv)
    stack_rows(tok_blocks, tok_rows, chips, nseq)
    for m in range(4):
        swapped(spots[m], query_w.at[pl.ds(pl.multiple_of(m * 2 * own + (1 - core) * own, own), own)], m)
    made = dot_turned(tok_rows[...], query_w[...])
    for i in range(chips):
        made_out[i] = made[i * nseq : (i + 1) * nseq].astype(bf16)
    made_in[chip] = made_out[chip]
    to_peer = lambda k: made_out.at[peers[k]]
    spread(to_peer, made_in, b_send, b_recv)
    arrive(to_peer, made_in, b_send, b_recv)

    lane = lax.broadcasted_iota(jnp.int32, (nseq, depth), 1)
    left = lane < depth // 2
    parts = ([], [], [], [])
    for h in range(heads):
        one, two = made_in[2 * h].astype(f32), made_in[2 * h + 1].astype(f32)
        for tile in range(2):
            a = one[:, tile * depth : (tile + 1) * depth]
            b = two[:, tile * depth : (tile + 1) * depth]
            parts[2 * tile].append(jnp.where(left, a, pltpu.roll(b, depth // 2, 1)))
            parts[2 * tile + 1].append(jnp.where(left, pltpu.roll(a, depth // 2, 1), b))
    query, forget_in, value, outgate = [jnp.concatenate(part, axis=0) for part in parts]
    forget = bounds + (1.0 - bounds) * jax.nn.sigmoid(forget_in)
    keyed = (1.0 - bounds) * jax.nn.sigmoid(-forget_in)
    aimed = query * forget
    overlap = jnp.sum(query * keyed, axis=1, keepdims=True)
    reads = []
    seq = lax.broadcasted_iota(jnp.int32, (2 * nseq, depth), 0) % nseq
    for p in range(heads // 2):
        pair = aimed[p * 2 * nseq : (p + 1) * 2 * nseq]
        zero = jnp.zeros((nseq, depth), f32)
        wide = jnp.concatenate(
            [jnp.concatenate([pair[:nseq], zero], axis=0), jnp.concatenate([zero, pair[nseq:]], axis=0)],
            axis=1,
        )
        high = wide.astype(bf16).astype(f32)
        lhs = jnp.concatenate([high, wide - high], axis=0).astype(bf16)
        read = jnp.zeros((2 * nseq, depth), f32)
        for q in range(nseq // 2):
            at = p * (nseq // 2) + q
            got = jnp.dot(lhs, state_high[at], preferred_element_type=f32)
            got = got + jnp.dot(lhs, state_low[at], preferred_element_type=f32)
            got = got[: 2 * nseq] + got[2 * nseq :]
            for b in range(2):
                read = jnp.where(seq == 2 * q + b, got[:, b * depth : (b + 1) * depth], read)
        reads.append(read)
    read = jnp.concatenate(reads, axis=0) + overlap * value
    scaled = read * lax.rsqrt(jnp.mean(jnp.square(read), axis=-1, keepdims=True) + HEAD_EPS) * head_gain[...]
    mixed = scaled * jax.nn.silu(outgate)
    mix_blocks[chip] = jnp.concatenate(
        [mixed[h * nseq : (h + 1) * nseq] for h in range(heads)], axis=1
    ).astype(bf16)
    own_mixed = lambda k: mix_blocks.at[chip]
    spread(own_mixed, mix_blocks, c_send, c_recv)

    tall = jnp.concatenate([forget, jnp.zeros((depth - heads * nseq, depth), f32)], axis=0).T
    for h in range(heads):
        for t in range(nseq):
            i = h * nseq + t
            here = value[i : i + 1]
            fresh_ref[t * heads + h] = here + tall[:, i : i + 1] * (state[t * heads + h] - here)

    arrive(own_mixed, mix_blocks, c_send, c_recv)
    stack_rows(mix_blocks, mix_rows, chips, nseq)
    swapped(mix_spot, mix_w.at[pl.ds(pl.multiple_of((1 - core) * mix_own, mix_own), mix_own)], 4)
    feats[chip] = dot_turned(mix_rows[...], mix_w[...]).astype(bf16)
    own_feats = lambda k: feats.at[chip]
    spread(own_feats, feats, d_send, d_recv)
    arrive(own_feats, feats, d_send, d_recv)

    for g in range(half // 16):
        rows = slice(g * 16, (g + 1) * 16)
        mixture = ALPHA * tok_rows[rows, :].astype(f32) + jnp.concatenate(
            [feats[c, rows, :].astype(f32) for c in range(chips)], axis=1
        )
        normed[rows, :] = layer_norm(mixture, first_gain[...], first_bias[...]).astype(bf16)
        swap(normed.at[rows], normed.at[half + g * 16 : half + (g + 1) * 16], 5 + g)
    for g in range(half // 16):
        rows = slice(g * 16, (g + 1) * 16)
        swapped(normed.at[rows], normed.at[half + g * 16 : half + (g + 1) * 16], 5 + g)
    swaps = 5 + half // 16

    x = normed[...]
    small = dot_turned(x, small_w[...])
    share = jax.nn.sigmoid(jnp.sum(small[:, :EXPERTS] * picks[:, :EXPERTS], axis=1, keepdims=True))
    branch_gate = jax.nn.sigmoid(small[:, EXPERTS : EXPERTS + 1])
    on_first = picks[:, EXPERTS : EXPERTS + 1] > 0
    on_second = picks[:, EXPERTS + 1 : EXPERTS + 2] > 0
    weight = jnp.where(on_first, share, jnp.where(on_second, 1.0 - share, 0.0))
    dot = functools.partial(jnp.dot, preferred_element_type=f32)
    for copy in get_dense:
        copy.wait()
    gate_part = dot_turned(x, dense_gate_w[...])
    up_part = dot_turned(x, dense_up_w[...])
    dense_hidden[...] = (jax.nn.silu(gate_part) * up_part).astype(bf16)
    for copy in get_wide:
        copy.wait()
    tile = column_tile(hidden.shape[1])
    for i in range(hidden.shape[1] // tile):
        at = slice(i * tile, (i + 1) * tile)
        gate_part = dot(normed[...], gate_w[:, at])
        up_part = dot(normed[...], up_w[:, at])
        hidden[:, at] = (jax.nn.silu(gate_part) * up_part).astype(bf16)
    for copy in get_down:
        copy.wait()

    step = width // chunks
    for j in range(chunks):
        tile = min(step, 256)
        for i in range(step // tile):
            at = slice(j * step + i * tile, j * step + (i + 1) * tile)
            routed = dot(hidden[...], down_w[:, at])
            dense = dot(dense_hidden[...], dense_down_w[:, at])
            made = branch_gate * dense + jnp.where(weight > 0, weight * routed, 0.0)
            own_part[:, at] = made[:half]
            pair_out[j, :, i * tile : (i + 1) * tile] = made[half:].astype(bf16)
        swap(pair_out.at[j], pair_in.at[j], swaps + j)
    for j in range(chunks):
        swapped(pair_out.at[j], pair_in.at[j], swaps + j)
        at = slice(j * step, (j + 1) * step)
        both = own_part[:, at] + pair_in[j].astype(f32)
        for i in range(chips):
            outgoing[j, i] = both[i * nseq : (i + 1) * nseq].astype(bf16)
        spread(lambda k: outgoing.at[j, peers[k]], landed.at[j], f_send.at[j], f_recv.at[j])
        landed[j, chip] = outgoing[j, chip]

    base = pl.multiple_of(lax.div(chip * nseq, 16) * 16, 16)
    around = normed[pl.ds(base, 16), :].astype(f32)
    place = lax.broadcasted_iota(jnp.int32, (16, width), 0) // nseq
    kept = jnp.where(place == lax.rem(chip, 16 // nseq), around, 0.0)
    residual = sum(kept[i * nseq : (i + 1) * nseq] for i in range(16 // nseq))
    sums = []
    for j in range(chunks):
        arrive(lambda k: outgoing.at[j, peers[k]], landed.at[j], f_send.at[j], f_recv.at[j])
        sums.append(sum(landed[j, i].astype(f32) for i in range(chips)))
    mixture = ALPHA * residual + jnp.concatenate(sums, axis=1)
    out_ref[...] = layer_norm(mixture, second_gain[...], second_bias[...]).astype(bf16)
    for copy in sent:
        copy.wait_send()


def fits(n, tokens, query_weight, mixout_weight, bound, depth):
    chips = n // 2
    nseq = tokens.shape[0]
    return (
        n % 2 == 0
        and chips & (chips - 1) == 0
        and n % EXPERTS == 0
        and nseq % 2 == 0
        and 16 % nseq == 0
        and (chips * nseq) % 16 == 0
        and 2 * mixout_weight.shape[1] == 128
        and 2 * query_weight.shape[1] == depth // 2
        and depth == 128
        and bound.shape[0] // depth * nseq <= depth
        and n * nseq == 128
        and tokens.shape[1] % 512 == 0
    )


def whole_layer(
    tokens, recurrent_state, query_weight, forget_weight, input_weight, outgate_weight,
    lower_bound, head_gain, mixout_weight, first_gain, first_bias, router_weight, branch_vector,
    dense_gate_weight, dense_up_weight, dense_down_weight, expert_gate_weight, expert_up_weight,
    expert_down_weight, second_gain, second_bias, routes,
):
    bf16, f32 = jnp.bfloat16, jnp.float32
    n = lax.axis_size("ep")
    chips = n // 2
    nseq, width = tokens.shape
    _, heads, depth, _ = recurrent_state.shape
    chunks = CHUNKS
    half = chips * nseq
    own, mix_own = query_weight.shape[1], mixout_weight.shape[1]
    operands = (
        tokens, recurrent_state.reshape(nseq * heads, depth, depth),
        query_weight.T, forget_weight.T, input_weight.T, outgate_weight.T,
        lower_bound.reshape(heads, depth), head_gain[None], mixout_weight.T,
        first_gain[None], first_bias[None], router_weight.T, branch_vector.reshape(-1, 128),
        dense_gate_weight.T, dense_up_weight.T, dense_down_weight,
        expert_gate_weight, expert_up_weight, expert_down_weight,
        second_gain[None], second_bias[None], routes.T,
    )
    (
        _, state, query, *_, bound, head, mix, gain1, bias1, router, branch,
        dgate, dup, ddown, gate, up, down, gain2, bias2, route,
    ) = operands
    vmem = lambda a: pltpu.VMEM(a.shape, a.dtype)
    sems = lambda *shape: pltpu.SemaphoreType.DMA(shape)
    pairs = 5 + half // 16 + chunks
    output, fresh = pl.pallas_call(
        functools.partial(layer_kernel, n, chunks),
        out_shape=(
            jax.ShapeDtypeStruct((nseq, width), bf16),
            jax.ShapeDtypeStruct(state.shape, f32),
        ),
        in_specs=[pl.BlockSpec(memory_space=pltpu.HBM)] * len(operands),
        out_specs=(pl.BlockSpec(memory_space=pltpu.VMEM), pl.BlockSpec(memory_space=pltpu.VMEM)),
        scratch_shapes=[
            vmem(state), pltpu.VMEM((8 * own, width), bf16),
            pltpu.VMEM((2 * mix_own, mix.shape[1]), bf16),
            *[vmem(a) for a in (gate, up, down, dgate, dup, ddown)],
            *[vmem(a) for a in (bound, head, gain1, bias1, router, branch, gain2, bias2, route)],
            pltpu.VMEM((chips, nseq, width), bf16), pltpu.VMEM((half, width), bf16),
            pltpu.VMEM((chips, nseq, 8 * own), bf16), pltpu.VMEM((chips, nseq, 8 * own), bf16),
            pltpu.VMEM((chips, nseq, mix.shape[1]), bf16), pltpu.VMEM((half, mix.shape[1]), bf16),
            pltpu.VMEM((chips, half, 2 * mix_own), bf16), pltpu.VMEM((2 * half, width), bf16),
            pltpu.VMEM((heads * nseq // 4, 2 * depth, 2 * depth), bf16),
            pltpu.VMEM((heads * nseq // 4, 2 * depth, 2 * depth), bf16),
            pltpu.VMEM((16, width), bf16),
            pltpu.VMEM((2 * half, gate.shape[1]), bf16), pltpu.VMEM((2 * half, dgate.shape[0]), bf16),
            pltpu.VMEM((half, width), f32),
            pltpu.VMEM((chunks, half, width // chunks), bf16),
            pltpu.VMEM((chunks, half, width // chunks), bf16),
            pltpu.VMEM((chunks, chips, nseq, width // chunks), bf16),
            pltpu.VMEM((chunks, chips, nseq, width // chunks), bf16),
            sems(len(operands)),
            *[sems(chips)] * 8, sems(chunks, chips), sems(chunks, chips), sems(pairs), sems(pairs),
        ],
        compiler_params=pltpu.CompilerParams(
            collective_id=3, has_side_effects=True, vmem_limit_bytes=44 * 2**20
        ),
    )(*operands)
    return output, fresh.reshape(recurrent_state.shape)


def per_device(
    tokens,
    recurrent_state,
    query_weight,
    forget_weight,
    input_weight,
    outgate_weight,
    lower_bound,
    head_gain,
    mixout_weight,
    first_gain,
    first_bias,
    router_weight,
    branch_vector,
    dense_gate_weight,
    dense_up_weight,
    dense_down_weight,
    expert_gate_weight,
    expert_up_weight,
    expert_down_weight,
    second_gain,
    second_bias,
    routes,
):
    f32 = jnp.float32
    devices = lax.axis_size("ep")
    if fits(
        devices, tokens, query_weight, mixout_weight, lower_bound, recurrent_state.shape[-1]
    ):
        return whole_layer(
            tokens, recurrent_state, query_weight, forget_weight, input_weight, outgate_weight,
            lower_bound, head_gain, mixout_weight, first_gain, first_bias, router_weight,
            branch_vector, dense_gate_weight, dense_up_weight, dense_down_weight,
            expert_gate_weight, expert_up_weight, expert_down_weight, second_gain, second_bias,
            routes,
        )
    nseq, width = tokens.shape
    own_cols = query_weight.shape[1]
    stacked = jnp.concatenate(
        [query_weight.T, forget_weight.T, input_weight.T, outgate_weight.T], axis=0
    )
    owned = project(tokens, stacked, devices, 0)
    projected = (
        owned.reshape(devices, nseq, 4, own_cols)
        .transpose(1, 2, 0, 3)
        .reshape(nseq, 4, devices * own_cols)
    )
    mixed, new_state = recurrence(projected, recurrent_state, lower_bound, head_gain)
    mix_out = project(mixed, mixout_weight.T, devices, 1).transpose(1, 0, 2).reshape(nseq, width)
    normed = layer_norm(
        ALPHA * tokens.astype(f32) + mix_out.astype(f32), first_gain, first_bias
    ).astype(jnp.bfloat16)
    output = channel_and_norm(
        normed,
        routes,
        devices,
        router_weight,
        branch_vector,
        dense_gate_weight,
        dense_up_weight,
        dense_down_weight,
        expert_gate_weight,
        expert_up_weight,
        expert_down_weight,
        second_gain,
        second_bias,
    )
    return (output, new_state)


def solution(mesh):
    return jax.shard_map(
        per_device,
        mesh=mesh,
        in_specs=(
            P("ep", None),
            P("ep", None, None, None),
            P(None, "ep"),
            P(None, "ep"),
            P(None, "ep"),
            P(None, "ep"),
            P(),
            P(),
            P(None, "ep"),
            P(),
            P(),
            P(),
            P(),
            P(None, "ep"),
            P(None, "ep"),
            P("ep", None),
            P(None, "ep"),
            P(None, "ep"),
            P("ep", None),
            P(),
            P(),
            P(),
        ),
        out_specs=(P("ep", None), P("ep", None, None, None)),
        check_vma=False,
    )
```

```python
import jax
import jax.numpy as jnp
from jax import lax
import functools

from jax.experimental import pallas as pl
from jax.experimental.pallas import tpu as pltpu
from jax.sharding import PartitionSpec as P

EXPERTS = 8
CHUNKS = 4
PLANE = 4
MESH = pl.DeviceIdType.MESH


ALPHA = 8.0**0.25
NORM_EPS = 1e-05
HEAD_EPS = 1e-06


def layer_norm(mixture, gain, bias):
    center = jnp.mean(mixture, axis=-1, keepdims=True)
    spread = jnp.mean(jnp.square(mixture - center), axis=-1, keepdims=True)
    return (mixture - center) * lax.rsqrt(spread + NORM_EPS) * gain + bias


def recurrence(projected, state, lower_bound, head_gain):
    nseq, heads, width = (state.shape[0], state.shape[1], state.shape[2])
    query = projected[:, 0].astype(jnp.float32).reshape(nseq, heads, width)
    forget_in = projected[:, 1].astype(jnp.float32)
    value = projected[:, 2].astype(jnp.float32).reshape(nseq, heads, width)
    outgate = projected[:, 3].astype(jnp.float32)
    forget = (lower_bound + (1.0 - lower_bound) * jax.nn.sigmoid(forget_in)).reshape(
        nseq, heads, width
    )
    keyed = ((1.0 - lower_bound) * jax.nn.sigmoid(-forget_in)).reshape(nseq, heads, width)
    fresh = forget[..., None] * state + keyed[..., None] * value[:, :, None, :]
    read = jnp.einsum("bhkv,bhk->bhv", fresh, query, precision=lax.Precision.HIGHEST)
    scaled = (
        read * lax.rsqrt(jnp.mean(jnp.square(read), axis=-1, keepdims=True) + HEAD_EPS) * head_gain
    )
    mixed = (scaled.reshape(nseq, heads * width) * jax.nn.silu(outgate)).astype(jnp.bfloat16)
    return (mixed, fresh)


def greet(n, me):
    barrier = pltpu.get_barrier_semaphore()

    @pl.loop(1, n)
    def _(k):
        pl.semaphore_signal(
            barrier, inc=1, device_id=(lax.rem(me + k, n),), device_id_type=MESH
        )

    pl.semaphore_wait(barrier, n - 1)


def start_all(source, dest, send_sem, recv_sem, n, me):
    @pl.loop(1, n)
    def _(k):
        peer = lax.rem(me + k, n)
        pltpu.make_async_remote_copy(
            src_ref=source(peer),
            dst_ref=dest.at[me],
            send_sem=send_sem.at[k],
            recv_sem=recv_sem.at[k],
            device_id=(peer,),
            device_id_type=MESH,
        ).start()


def wait_all(source, dest, send_sem, recv_sem, n, me):
    @pl.loop(1, n)
    def _(k):
        peer = lax.rem(me + k, n)
        pltpu.make_async_remote_copy(
            src_ref=source(peer),
            dst_ref=dest.at[lax.rem(me + n - k, n)],
            send_sem=send_sem.at[k],
            recv_sem=recv_sem.at[k],
            device_id=(peer,),
            device_id_type=MESH,
        ).wait()


def gather_all(block_ref, gathered, send_sem, recv_sem, n, me):
    chips = n // 2
    chip, core = lax.div(me, 2), lax.rem(me, 2)
    sibling = 2 * chip + 1 - core

    def across(k, owner):
        return pltpu.make_async_remote_copy(
            src_ref=block_ref,
            dst_ref=gathered.at[owner],
            send_sem=send_sem.at[k],
            recv_sem=recv_sem.at[k],
            device_id=(2 * lax.rem(chip + k, chips) + core,),
            device_id_type=MESH,
        )

    def onward(k, source, owner):
        return pltpu.make_async_remote_copy(
            src_ref=source,
            dst_ref=gathered.at[owner],
            send_sem=send_sem.at[chips + k],
            recv_sem=recv_sem.at[chips + k],
            device_id=(sibling,),
            device_id_type=MESH,
        )

    pl.loop(1, chips)(lambda k: across(k, me).start())
    onward(0, block_ref, me).start()
    gathered[me] = block_ref[...]

    @pl.loop(1, chips)
    def _(k):
        owner = 2 * lax.rem(chip + chips - k, chips) + core
        across(k, owner).wait()
        onward(k, gathered.at[owner], owner).start()

    onward(0, block_ref, sibling).wait()

    @pl.loop(1, chips)
    def _(k):
        base = 2 * lax.rem(chip + chips - k, chips)
        onward(k, gathered.at[base + core], base + 1 - core).wait()


def dot_turned(rows, weight):
    return lax.dot_general(
        rows, weight, (((1,), (1,)), ((), ())), preferred_element_type=jnp.float32
    )


def flatten_rows(blocks, flat, n, nseq):
    group = max(1, 16 // nseq)

    @pl.loop(0, n // group)
    def _(i):
        parts = [blocks[i * group + j].astype(jnp.float32) for j in range(group)]
        at = pl.multiple_of(i * (group * nseq), group * nseq)
        flat[pl.ds(at, group * nseq), :] = jnp.concatenate(parts, axis=0).astype(flat.dtype)


def split_rows(flat, blocks, n, nseq):
    group = max(1, 8 // nseq)

    @pl.loop(0, n // group)
    def _(i):
        at = pl.multiple_of(i * (group * nseq), group * nseq)
        taken = flat[pl.ds(at, group * nseq), :]
        for j in range(group):
            blocks[i * group + j] = taken[j * nseq : (j + 1) * nseq].astype(blocks.dtype)


def project_kernel(
    n, block_ref, weight_hbm, out_ref,
    weight, gathered, rows, made, outgoing, landed,
    weight_sem, gather_send, gather_recv, back_send, back_recv,
):
    me = lax.axis_index("ep")
    nseq = block_ref.shape[0]
    load = pltpu.make_async_copy(weight_hbm, weight, weight_sem)
    load.start()
    greet(n, me)
    gather_all(block_ref, gathered, gather_send, gather_recv, n, me)
    flatten_rows(gathered, rows, n, nseq)
    load.wait()
    made[...] = dot_turned(rows[...], weight[...])
    split_rows(made, outgoing, n, nseq)
    part = lambda peer: outgoing.at[peer]
    start_all(part, landed, back_send, back_recv, n, me)
    landed[me] = outgoing[me]
    wait_all(part, landed, back_send, back_recv, n, me)
    out_ref[...] = landed[...]


def exchange_semaphores(n):
    return [pltpu.SemaphoreType.DMA((n,))] * 4


def project(block, weight, n, collective_id):
    nseq, width = block.shape
    cols = weight.shape[0]
    bf16, f32 = jnp.bfloat16, jnp.float32
    return pl.pallas_call(
        functools.partial(project_kernel, n),
        out_shape=jax.ShapeDtypeStruct((n, nseq, cols), bf16),
        in_specs=[
            pl.BlockSpec(memory_space=pltpu.VMEM),
            pl.BlockSpec(memory_space=pl.ANY),
        ],
        out_specs=pl.BlockSpec(memory_space=pltpu.VMEM),
        scratch_shapes=[
            pltpu.VMEM(weight.shape, bf16),
            pltpu.VMEM((n, nseq, width), bf16),
            pltpu.VMEM((n * nseq, width), bf16),
            pltpu.VMEM((n * nseq, cols), f32),
            pltpu.VMEM((n, nseq, cols), bf16),
            pltpu.VMEM((n, nseq, cols), bf16),
            pltpu.SemaphoreType.DMA,
            *exchange_semaphores(n),
        ],
        compiler_params=pltpu.CompilerParams(
            collective_id=collective_id, has_side_effects=True, vmem_limit_bytes=24 * 2**20
        ),
    )(block, weight)


def column_tile(cols):
    return 256 if cols % 256 == 0 else cols


def for_tiles(cols, body):
    tile = column_tile(cols)
    if tile == cols:
        body(slice(None))
    else:
        pl.loop(0, cols // tile)(lambda i: body(pl.ds(pl.multiple_of(i * tile, tile), tile)))


def channel_kernel(
    n, block_ref, pick_ref, small_ref, gain_ref, bias_ref,
    gate_hbm, up_hbm, down_hbm, dense_gate_hbm, dense_up_hbm, dense_down_hbm, out_ref,
    gate_w, up_w, down_w, dense_gate_w, dense_up_w, dense_down_w,
    gathered, rows, hidden, dense_hidden, made, outgoing, landed,
    weight_sem, gather_send, gather_recv, back_send, back_recv,
):
    f32 = jnp.float32
    me = lax.axis_index("ep")
    nseq, width = block_ref.shape
    pairs = (
        (dense_gate_hbm, dense_gate_w),
        (dense_up_hbm, dense_up_w),
        (gate_hbm, gate_w),
        (up_hbm, up_w),
        (dense_down_hbm, dense_down_w),
        (down_hbm, down_w),
    )
    loads = [
        pltpu.make_async_copy(there, here, weight_sem.at[i]) for i, (there, here) in enumerate(pairs)
    ]
    for load in loads:
        load.start()
    greet(n, me)
    gather_all(block_ref, gathered, gather_send, gather_recv, n, me)
    flatten_rows(gathered, rows, n, nseq)
    dot = functools.partial(jnp.dot, preferred_element_type=f32)

    small = dot_turned(rows[...], small_ref[...])
    picks = pick_ref[...]
    logit_gap = jnp.sum(small[:, :EXPERTS] * picks[:, :EXPERTS], axis=1, keepdims=True)
    share = jax.nn.sigmoid(logit_gap)
    branch_gate = jax.nn.sigmoid(small[:, EXPERTS : EXPERTS + 1])
    on_first = picks[:, EXPERTS : EXPERTS + 1] > 0
    on_second = picks[:, EXPERTS + 1 : EXPERTS + 2] > 0
    weight = jnp.where(on_first, share, jnp.where(on_second, 1.0 - share, 0.0))

    def fill(target, gate, up):
        def body(at):
            gate_part = dot(rows[...], gate[:, at])
            up_part = dot(rows[...], up[:, at])
            target[:, at] = (jax.nn.silu(gate_part) * up_part).astype(jnp.bfloat16)

        for_tiles(target.shape[1], body)

    for load in loads[:2]:
        load.wait()
    gate_part = dot_turned(rows[...], dense_gate_w[...])
    up_part = dot_turned(rows[...], dense_up_w[...])
    dense_hidden[...] = (jax.nn.silu(gate_part) * up_part).astype(jnp.bfloat16)
    for load in loads[2:4]:
        load.wait()
    fill(hidden, gate_w, up_w)
    for load in loads[4:]:
        load.wait()

    def down(at):
        routed = dot(hidden[...], down_w[:, at])
        dense = dot(dense_hidden[...], dense_down_w[:, at])
        made[:, at] = branch_gate * dense + jnp.where(weight > 0, weight * routed, 0.0)

    for_tiles(width, down)
    split_rows(made, outgoing, n, nseq)
    part = lambda peer: outgoing.at[peer]
    start_all(part, landed, back_send, back_recv, n, me)
    landed[me] = outgoing[me]
    wait_all(part, landed, back_send, back_recv, n, me)
    channel = lax.fori_loop(
        0, n, lambda d, total: total + landed[d].astype(f32), jnp.zeros((nseq, width), f32)
    )
    mixture = ALPHA * block_ref[...].astype(f32) + channel
    out_ref[...] = layer_norm(mixture, gain_ref[...], bias_ref[...]).astype(jnp.bfloat16)


def channel_and_norm(
    normed, routes, n, router_weight, branch_vector, dense_gate_weight, dense_up_weight,
    dense_down_weight, expert_gate_weight, expert_up_weight, expert_down_weight, gain, bias,
):
    bf16, f32 = jnp.bfloat16, jnp.float32
    nseq, width = normed.shape
    total = n * nseq
    expert = lax.axis_index("ep") // (n // EXPERTS)
    first = jax.nn.one_hot(routes[:, 0], EXPERTS, dtype=f32)
    second = jax.nn.one_hot(routes[:, 1], EXPERTS, dtype=f32)
    picks = jnp.concatenate([first - second, (routes == expert).astype(f32)], axis=1)
    small = jnp.concatenate([router_weight.T, branch_vector[None]], axis=0)
    weights = (
        expert_gate_weight,
        expert_up_weight,
        expert_down_weight,
        dense_gate_weight.T,
        dense_up_weight.T,
        dense_down_weight,
    )
    vmem, anywhere = pl.BlockSpec(memory_space=pltpu.VMEM), pl.BlockSpec(memory_space=pl.ANY)
    return pl.pallas_call(
        functools.partial(channel_kernel, n),
        out_shape=jax.ShapeDtypeStruct((nseq, width), bf16),
        in_specs=[vmem] * 5 + [anywhere] * 6,
        out_specs=vmem,
        scratch_shapes=[
            *[pltpu.VMEM(w.shape, bf16) for w in weights],
            pltpu.VMEM((n, nseq, width), bf16),
            pltpu.VMEM((total, width), bf16),
            pltpu.VMEM((total, expert_gate_weight.shape[1]), bf16),
            pltpu.VMEM((total, dense_gate_weight.shape[1]), bf16),
            pltpu.VMEM((total, width), f32),
            pltpu.VMEM((n, nseq, width), bf16),
            pltpu.VMEM((n, nseq, width), bf16),
            pltpu.SemaphoreType.DMA((6,)),
            *exchange_semaphores(n),
        ],
        compiler_params=pltpu.CompilerParams(
            collective_id=2, has_side_effects=True, vmem_limit_bytes=56 * 2**20
        ),
    )(normed, picks, small, gain[None], bias[None], *weights)


def parity_peers(chip, chips):
    bits = [1 << i for i in range(chips.bit_length() - 1)]
    steps = [(1 - 2 * lax.rem(lax.div(chip, bit), 2)) * bit for bit in bits]
    peers = []
    for k in range(chips):
        peer = chip
        for bit, step in zip(bits, steps):
            if k & bit:
                peer = peer + step
        peers.append(peer)
    return peers


def remote(source, dest, send_sem, recv_sem, device):
    return pltpu.make_async_remote_copy(
        src_ref=source, dst_ref=dest, send_sem=send_sem, recv_sem=recv_sem,
        device_id=(device,), device_id_type=MESH,
    )


def stack_rows(blocks, flat, chips, nseq):
    group = 16 // nseq
    for i in range(chips // group):
        parts = [blocks[i * group + j].astype(jnp.float32) for j in range(group)]
        flat[i * 16 : (i + 1) * 16, :] = jnp.concatenate(parts, axis=0).astype(flat.dtype)


def layer_kernel(
    n, chunks,
    tokens_hbm, state_hbm, query_hbm, forget_hbm, value_hbm, outgate_hbm, bound_hbm, head_gain_hbm,
    mixout_hbm, first_gain_hbm, first_bias_hbm, router_hbm, branch_hbm,
    dense_gate_hbm, dense_up_hbm, dense_down_hbm, gate_hbm, up_hbm, down_hbm,
    routes_hbm,
    out_ref, fresh_ref,
    state, query_w, mix_w, wide_w, down_w, dense_w, dense_down_w,
    bound, head_gain, first_gain, first_bias, router, branch, routes,
    tok_blocks, tok_rows, made_out, made_in, mix_blocks, mix_rows, feats, stretched, normed,
    state_high, state_low, small_w, hidden, dense_hidden, own_part, pair_out, pair_in,
    outgoing, landed,
    ready, load_sem, a_send, a_recv, b_send, b_recv, c_send, c_recv, d_send, d_recv, f_send, f_recv,
    pair_send, pair_recv,
):
    bf16, f32 = jnp.bfloat16, jnp.float32
    me = lax.axis_index("ep")
    chips = n // 2
    chip, core = lax.div(me, 2), lax.rem(me, 2)
    sibling = 2 * chip + 1 - core
    peers = parity_peers(chip, chips)
    devices = [2 * peer + core for peer in peers]
    order = list(range(chips - 1, 0, -1))
    nseq, width = tokens_hbm.shape
    heads, depth = bound.shape
    half = chips * nseq
    own = query_hbm.shape[0]
    mix_own = mixout_hbm.shape[0]
    at_core = lambda base, size: pl.ds(pl.multiple_of(base + core * size, size), size)

    def load(there, here, i):
        copy = pltpu.make_async_copy(there, here, load_sem.at[i])
        copy.start()
        return copy

    def drain(ref, sem):
        pltpu.make_async_copy(ref, ref, sem).wait()

    get_tokens = load(tokens_hbm, tok_blocks.at[chip], 0)
    pieces = (query_hbm, forget_hbm, value_hbm, outgate_hbm)
    spots = [query_w.at[at_core(m * 2 * own, own)] for m in range(4)]
    for piece, spot in zip(pieces, spots):
        load(piece, spot, 1)
    mix_spot = mix_w.at[at_core(0, mix_own)]
    get_mix = load(mixout_hbm, mix_spot, 2)
    get_state = load(state_hbm, state, 3)
    get_small = [
        load(there, here, 4 + i)
        for i, (there, here) in enumerate((
            (bound_hbm, bound), (head_gain_hbm, head_gain), (first_gain_hbm, first_gain),
            (first_bias_hbm, first_bias), (router_hbm, router), (branch_hbm, branch),
            (routes_hbm, routes),
        ))
    ]
    load(dense_gate_hbm, dense_w.at[0], 11)
    load(dense_up_hbm, dense_w.at[1], 11)
    load(gate_hbm, wide_w.at[0], 12)
    load(up_hbm, wide_w.at[1], 12)
    get_down = [load(dense_down_hbm, dense_down_w, 13), load(down_hbm, down_w, 14)]

    barrier = pltpu.get_barrier_semaphore()
    above = [peer > chip for peer in peers]
    partners = [k for k in range(1, chips) if k < PLANE or k % PLANE == 0]
    pl.semaphore_signal(barrier, inc=1, device_id=(sibling,), device_id_type=MESH)
    for k in partners:

        @pl.when(above[k])
        def _(k=k):
            pl.semaphore_signal(barrier, inc=1, device_id=(devices[k],), device_id_type=MESH)

    pl.semaphore_wait(barrier, lax.div(chip, PLANE) + lax.rem(chip, PLANE) + 1)
    for k in partners:

        @pl.when(jnp.logical_not(above[k]))
        def _(k=k):
            pl.semaphore_signal(ready.at[partners.index(k)], inc=1, device_id=(devices[k],), device_id_type=MESH)

    sent = []

    def spread(source, dest, send_sem, recv_sem):
        for k in order:
            remote(source(k), dest.at[chip], send_sem, recv_sem, devices[k]).start()
        sent.append((dest.at[: chips - 1], send_sem))

    def arrive(dest, recv_sem):
        drain(dest.at[: chips - 1], recv_sem)

    lines = range(PLANE, chips, PLANE)
    others = chips // PLANE * (PLANE - 1)

    def step_copy(blocks, send_sem, recv_sem, line, k, device=None):
        block = blocks.at[peers[line]]
        device = devices[k] if device is None else device
        return remote(block, block, send_sem, recv_sem.at[k // PLANE], device)

    def landing(blocks, send_sem, recv_sem, line):
        remote(
            blocks.at[chip], blocks.at[peers[line]], send_sem, recv_sem.at[line // PLANE], devices[line]
        ).wait_recv()

    def onward(blocks, send_sem, recv_sem):
        for line in lines:
            landing(blocks, send_sem, recv_sem, line)
            for k in range(1, PLANE):
                step_copy(blocks, send_sem, recv_sem, line, k).start()

    def swap(source, dest, i):
        remote(source, dest, pair_send.at[i], pair_recv.at[i], sibling).start()

    get_tokens.wait()
    for k in reversed(partners):

        @pl.when(jnp.logical_not(above[k]))
        def _(k=k):
            step_copy(tok_blocks, a_send, a_recv, 0, k).start()

    for k in partners:

        @pl.when(above[k])
        def _(k=k):
            pl.semaphore_wait(ready.at[partners.index(k)], 1)
            step_copy(tok_blocks, a_send, a_recv, 0, k).start()
    drain(query_w.at[: 4 * own], load_sem.at[1])
    for m in range(4):
        swap(spots[m], spots[m], 0)
    sent.append((query_w.at[: 4 * own], pair_send.at[0]))
    get_mix.wait()
    swap(mix_spot, mix_spot, 1)
    sent.append((mix_spot, pair_send.at[1]))

    onward(tok_blocks, a_send, a_recv)
    sent.append((tok_blocks.at[: chips - 1], a_send))

    for copy in get_small:
        copy.wait()
    spread_rows = lambda rows: jnp.concatenate(
        [jnp.broadcast_to(rows[h : h + 1], (nseq, depth)) for h in range(heads)], axis=0
    )
    bounds = spread_rows(bound[...])
    branch_row = jnp.concatenate([branch[i : i + 1, :].astype(f32) for i in range(branch.shape[0])], axis=1)
    small_w[...] = jnp.concatenate(
        [router[...].astype(f32), branch_row, jnp.zeros((16 - EXPERTS - 1, width), f32)], axis=0
    ).astype(bf16)

    total = n * nseq
    expert = lax.div(me, n // EXPERTS)
    first, second = routes[0:1, :], routes[1:2, :]
    ids = lax.broadcasted_iota(jnp.int32, (EXPERTS, total), 0)
    gap = (first == ids).astype(f32) - (second == ids).astype(f32)
    table = jnp.concatenate(
        [gap, (first == expert).astype(f32), (second == expert).astype(f32),
         jnp.zeros((16 - EXPERTS - 2, total), f32)], axis=0,
    ).astype(bf16)
    row = lax.broadcasted_iota(jnp.int32, (total, total), 0)
    column = lax.broadcasted_iota(jnp.int32, (total, total), 1)
    local = jnp.where(row < half, row, row - half)
    parity = jnp.where(row < half, core, 1 - core)
    which = (2 * (local // nseq) + parity) * nseq + local % nseq
    turn = (which == column).astype(f32).astype(bf16)
    picks = dot_turned(turn, table)

    get_state.wait()
    for p in range(heads // 2):
        for q in range(nseq // 2):
            for a in range(2):
                for b in range(2):
                    block = state[(2 * q + b) * heads + 2 * p + a]
                    high = block.astype(bf16)
                    low = (block - high.astype(f32)).astype(bf16)
                    at = (p * (nseq // 2) + q, slice(a * depth, (a + 1) * depth), slice(b * depth, (b + 1) * depth))
                    state_high[at] = high
                    state_low[at] = low

    drain(tok_blocks.at[:others], a_recv.at[0])
    stack_rows(tok_blocks, tok_rows, chips, nseq)
    drain(query_w.at[: 4 * own], pair_recv.at[0])
    made = dot_turned(tok_rows[...], query_w[...])
    for i in range(chips):
        made_out[i] = made[i * nseq : (i + 1) * nseq].astype(bf16)
    made_in[chip] = made_out[chip]
    to_peer = lambda k: made_out.at[peers[k]]
    spread(to_peer, made_in, b_send, b_recv)
    stretched[...] = ALPHA * tok_rows[...].astype(f32)
    arrive(made_in, b_recv)

    lane = lax.broadcasted_iota(jnp.int32, (nseq, depth), 1)
    left = lane < depth // 2
    parts = ([], [], [], [])
    for h in range(heads):
        one, two = made_in[2 * h].astype(f32), made_in[2 * h + 1].astype(f32)
        for tile in range(2):
            a = one[:, tile * depth : (tile + 1) * depth]
            b = two[:, tile * depth : (tile + 1) * depth]
            parts[2 * tile].append(jnp.where(left, a, pltpu.roll(b, depth // 2, 1)))
            parts[2 * tile + 1].append(jnp.where(left, pltpu.roll(a, depth // 2, 1), b))
    query, forget_in, value, outgate = [jnp.concatenate(part, axis=0) for part in parts]
    forget = bounds + (1.0 - bounds) * jax.nn.sigmoid(forget_in)
    keyed = (1.0 - bounds) * jax.nn.sigmoid(-forget_in)
    aimed = query * forget
    overlap = jnp.sum(query * keyed, axis=1, keepdims=True)
    reads = []
    seq = lax.broadcasted_iota(jnp.int32, (2 * nseq, depth), 0) % nseq
    for p in range(heads // 2):
        pair = aimed[p * 2 * nseq : (p + 1) * 2 * nseq]
        zero = jnp.zeros((nseq, depth), f32)
        wide = jnp.concatenate(
            [jnp.concatenate([pair[:nseq], zero], axis=0), jnp.concatenate([zero, pair[nseq:]], axis=0)],
            axis=1,
        )
        high = wide.astype(bf16).astype(f32)
        lhs = jnp.concatenate([high, wide - high], axis=0).astype(bf16)
        read = jnp.zeros((2 * nseq, depth), f32)
        for q in range(nseq // 2):
            at = p * (nseq // 2) + q
            got = jnp.dot(lhs, state_high[at], preferred_element_type=f32)
            got = got + jnp.dot(lhs, state_low[at], preferred_element_type=f32)
            got = got[: 2 * nseq] + got[2 * nseq :]
            for b in range(2):
                read = jnp.where(seq == 2 * q + b, got[:, b * depth : (b + 1) * depth], read)
        reads.append(read)
    read = jnp.concatenate(reads, axis=0) + overlap * value
    scaled = read * lax.rsqrt(jnp.mean(jnp.square(read), axis=-1, keepdims=True) + HEAD_EPS) * head_gain[...]
    mixed = scaled * jax.nn.silu(outgate)
    mix_blocks[chip] = jnp.concatenate(
        [mixed[h * nseq : (h + 1) * nseq] for h in range(heads)], axis=1
    ).astype(bf16)
    own_mixed = lambda k: mix_blocks.at[chip]
    spread(own_mixed, mix_blocks, c_send, c_recv)

    tall = jnp.concatenate([forget, jnp.zeros((depth - heads * nseq, depth), f32)], axis=0).T
    for h in range(heads):
        for t in range(nseq):
            i = h * nseq + t
            here = value[i : i + 1]
            fresh_ref[t * heads + h] = here + tall[:, i : i + 1] * (state[t * heads + h] - here)

    arrive(mix_blocks, c_recv)
    stack_rows(mix_blocks, mix_rows, chips, nseq)
    drain(mix_spot, pair_recv.at[1])
    feats[chip] = dot_turned(mix_rows[...], mix_w[...]).astype(bf16)
    @pl.when(core == 1)
    def _():
        for k in partners:
            step_copy(feats, d_send, d_recv, 0, k).start()
        onward(feats, d_send, d_recv)

    @pl.when(core == 0)
    def _():
        for k in order:
            step_copy(feats, d_send, d_recv, 0, k if k % PLANE == 0 else k % PLANE, devices[k]).start()
        for line in lines:
            landing(feats, d_send, d_recv, line)

    sent.append((feats.at[: chips - 1], d_send))

    lanes = 2 * mix_own

    def take(c):
        at = pl.ds(pl.multiple_of(c * lanes, lanes), lanes)
        value = stretched[:, at] + feats[c].astype(f32)
        stretched[:, at] = value
        return value

    total = take(chip)
    for line in lines:
        total = total + take(peers[line])
    drain(feats.at[:others], d_recv.at[0])
    for k in range(1, chips):
        if k % PLANE:
            total = total + take(peers[k])
    center = jnp.sum(total, axis=1, keepdims=True) * (1.0 / width)
    groups = [slice(g * 16, (g + 1) * 16) for g in range(half // 16)]
    spreads = [
        lax.rsqrt(
            jnp.mean(jnp.square(stretched[rows, :] - center[rows]), axis=1, keepdims=True) + NORM_EPS
        )
        for rows in groups
    ]
    for g, rows in enumerate(groups):
        row = (stretched[rows, :] - center[rows]) * spreads[g] * first_gain[...] + first_bias[...]
        normed[rows, :] = row.astype(bf16)
        swap(normed.at[rows], normed.at[half + g * 16 : half + (g + 1) * 16], 2)
    sent.append((normed.at[:half], pair_send.at[2]))
    drain(normed.at[half:], pair_recv.at[2])

    x = normed[...]
    small = dot_turned(x, small_w[...])
    share = jax.nn.sigmoid(jnp.sum(small[:, :EXPERTS] * picks[:, :EXPERTS], axis=1, keepdims=True))
    branch_gate = jax.nn.sigmoid(small[:, EXPERTS : EXPERTS + 1])
    on_first = picks[:, EXPERTS : EXPERTS + 1] > 0
    on_second = picks[:, EXPERTS + 1 : EXPERTS + 2] > 0
    weight = jnp.where(on_first, share, jnp.where(on_second, 1.0 - share, 0.0))
    dot = functools.partial(jnp.dot, preferred_element_type=f32)
    drain(dense_w, load_sem.at[11])
    gate_part = dot_turned(x, dense_w[0])
    up_part = dot_turned(x, dense_w[1])
    dense_hidden[...] = (jax.nn.silu(gate_part) * up_part).astype(bf16)
    drain(wide_w, load_sem.at[12])
    tile = column_tile(hidden.shape[1])
    for i in range(hidden.shape[1] // tile):
        at = slice(i * tile, (i + 1) * tile)
        gate_part = dot(normed[...], wide_w[0, :, at])
        up_part = dot(normed[...], wide_w[1, :, at])
        hidden[:, at] = (jax.nn.silu(gate_part) * up_part).astype(bf16)
    for copy in get_down:
        copy.wait()

    step = width // chunks
    for j in range(chunks):
        tile = min(step, 256)
        for i in range(step // tile):
            at = slice(j * step + i * tile, j * step + (i + 1) * tile)
            routed = dot(hidden[...], down_w[:, at])
            dense = dot(dense_hidden[...], dense_down_w[:, at])
            made = branch_gate * dense + jnp.where(weight > 0, weight * routed, 0.0)
            own_part[:, at] = made[:half]
            pair_out[j, :, i * tile : (i + 1) * tile] = made[half:].astype(bf16)
        swap(pair_out.at[j], pair_in.at[j], 3 + j)
        sent.append((pair_out.at[j], pair_send.at[3 + j]))
    for j in range(chunks):
        drain(pair_in.at[j], pair_recv.at[3 + j])
        at = slice(j * step, (j + 1) * step)
        both = own_part[:, at] + pair_in[j].astype(f32)
        for i in range(chips):
            outgoing[j, i] = both[i * nseq : (i + 1) * nseq].astype(bf16)
        spread(lambda k: outgoing.at[j, peers[k]], landed.at[j], f_send.at[j], f_recv.at[j])
        landed[j, chip] = outgoing[j, chip]

    base = pl.multiple_of(lax.div(chip * nseq, 16) * 16, 16)
    around = normed[pl.ds(base, 16), :].astype(f32)
    place = lax.broadcasted_iota(jnp.int32, (16, width), 0) // nseq
    kept = jnp.where(place == lax.rem(chip, 16 // nseq), around, 0.0)
    residual = sum(kept[i * nseq : (i + 1) * nseq] for i in range(16 // nseq))
    sums = []
    for j in range(chunks):
        arrive(landed.at[j], f_recv.at[j])
        sums.append(sum(landed[j, i].astype(f32) for i in range(chips)))
    mixture = ALPHA * residual + jnp.concatenate(sums, axis=1)
    out_ref[...] = mixture
    for ref, sem in sent:
        drain(ref, sem)


def finish_kernel(mixture, fresh, gain, bias, out_hbm, state_hbm, rows, sem):
    keep = pltpu.make_async_copy(fresh, state_hbm, sem.at[0])
    keep.start()
    rows[...] = layer_norm(mixture[...], gain[...], bias[...]).astype(rows.dtype)
    give = pltpu.make_async_copy(rows, out_hbm, sem.at[1])
    give.start()
    give.wait()
    keep.wait()


def fits(n, tokens, query_weight, mixout_weight, bound, depth):
    chips = n // 2
    nseq = tokens.shape[0]
    return (
        n % 2 == 0
        and chips & (chips - 1) == 0
        and n % EXPERTS == 0
        and nseq % 2 == 0
        and 16 % nseq == 0
        and (chips * nseq) % 16 == 0
        and 2 * mixout_weight.shape[1] == 128
        and 2 * query_weight.shape[1] == depth // 2
        and depth == 128
        and bound.shape[0] // depth * nseq <= depth
        and n * nseq == 128
        and tokens.shape[1] % 512 == 0
    )


def whole_layer(
    tokens, recurrent_state, query_weight, forget_weight, input_weight, outgate_weight,
    lower_bound, head_gain, mixout_weight, first_gain, first_bias, router_weight, branch_vector,
    dense_gate_weight, dense_up_weight, dense_down_weight, expert_gate_weight, expert_up_weight,
    expert_down_weight, second_gain, second_bias, routes,
):
    bf16, f32 = jnp.bfloat16, jnp.float32
    n = lax.axis_size("ep")
    chips = n // 2
    nseq, width = tokens.shape
    _, heads, depth, _ = recurrent_state.shape
    chunks = CHUNKS
    half = chips * nseq
    own, mix_own = query_weight.shape[1], mixout_weight.shape[1]
    operands = (
        tokens, recurrent_state.reshape(nseq * heads, depth, depth),
        query_weight.T, forget_weight.T, input_weight.T, outgate_weight.T,
        lower_bound.reshape(heads, depth), head_gain[None], mixout_weight.T,
        first_gain[None], first_bias[None], router_weight.T, branch_vector.reshape(-1, 128),
        dense_gate_weight.T, dense_up_weight.T, dense_down_weight,
        expert_gate_weight, expert_up_weight, expert_down_weight,
        routes.T,
    )
    (
        _, state, query, *_, bound, head, mix, gain1, bias1, router, branch,
        dgate, dup, ddown, gate, up, down, route,
    ) = operands
    vmem = lambda a: pltpu.VMEM(a.shape, a.dtype)
    sems = lambda *shape: pltpu.SemaphoreType.DMA(shape)
    one = pltpu.SemaphoreType.DMA
    mixture, fresh = pl.pallas_call(
        functools.partial(layer_kernel, n, chunks),
        out_shape=(
            jax.ShapeDtypeStruct((nseq, width), f32),
            jax.ShapeDtypeStruct(state.shape, f32),
        ),
        in_specs=[pl.BlockSpec(memory_space=pltpu.HBM)] * len(operands),
        out_specs=(pl.BlockSpec(memory_space=pltpu.VMEM), pl.BlockSpec(memory_space=pltpu.VMEM)),
        scratch_shapes=[
            vmem(state), pltpu.VMEM((8 * own, width), bf16),
            pltpu.VMEM((2 * mix_own, mix.shape[1]), bf16),
            pltpu.VMEM((2, *gate.shape), bf16), vmem(down), pltpu.VMEM((2, *dgate.shape), bf16), vmem(ddown),
            *[vmem(a) for a in (bound, head, gain1, bias1, router, branch, route)],
            pltpu.VMEM((chips, nseq, width), bf16), pltpu.VMEM((half, width), bf16),
            pltpu.VMEM((chips, nseq, 8 * own), bf16), pltpu.VMEM((chips, nseq, 8 * own), bf16),
            pltpu.VMEM((chips, nseq, mix.shape[1]), bf16), pltpu.VMEM((half, mix.shape[1]), bf16),
            pltpu.VMEM((chips, half, 2 * mix_own), bf16), pltpu.VMEM((half, width), f32),
            pltpu.VMEM((2 * half, width), bf16),
            pltpu.VMEM((heads * nseq // 4, 2 * depth, 2 * depth), bf16),
            pltpu.VMEM((heads * nseq // 4, 2 * depth, 2 * depth), bf16),
            pltpu.VMEM((16, width), bf16),
            pltpu.VMEM((2 * half, gate.shape[1]), bf16), pltpu.VMEM((2 * half, dgate.shape[0]), bf16),
            pltpu.VMEM((half, width), f32),
            pltpu.VMEM((chunks, half, width // chunks), bf16),
            pltpu.VMEM((chunks, half, width // chunks), bf16),
            pltpu.VMEM((chunks, chips, nseq, width // chunks), bf16),
            pltpu.VMEM((chunks, chips, nseq, width // chunks), bf16),
            pltpu.SemaphoreType.REGULAR((PLANE - 1 + chips // PLANE - 1,)), sems(15),
            one, sems(chips // PLANE), one, one, one, one, one, sems(chips // PLANE),
            sems(chunks), sems(chunks), sems(3 + chunks), sems(3 + chunks),
        ],
        compiler_params=pltpu.CompilerParams(
            collective_id=3, has_side_effects=True, vmem_limit_bytes=44 * 2**20
        ),
    )(*[pltpu.with_memory_space_constraint(a, pltpu.HBM) for a in operands])
    anywhere, here = pl.BlockSpec(memory_space=pl.ANY), pl.BlockSpec(memory_space=pltpu.VMEM)
    output, new_state = pl.pallas_call(
        finish_kernel,
        out_shape=(
            jax.ShapeDtypeStruct((nseq, width), bf16),
            jax.ShapeDtypeStruct(state.shape, f32),
        ),
        in_specs=[here] * 4,
        out_specs=(anywhere, anywhere),
        scratch_shapes=[pltpu.VMEM((nseq, width), bf16), sems(2)],
        compiler_params=pltpu.CompilerParams(vmem_limit_bytes=4 * 2**20),
    )(mixture, fresh, second_gain[None], second_bias[None])
    return output, new_state.reshape(recurrent_state.shape)


def per_device(
    tokens,
    recurrent_state,
    query_weight,
    forget_weight,
    input_weight,
    outgate_weight,
    lower_bound,
    head_gain,
    mixout_weight,
    first_gain,
    first_bias,
    router_weight,
    branch_vector,
    dense_gate_weight,
    dense_up_weight,
    dense_down_weight,
    expert_gate_weight,
    expert_up_weight,
    expert_down_weight,
    second_gain,
    second_bias,
    routes,
):
    f32 = jnp.float32
    devices = lax.axis_size("ep")
    if fits(
        devices, tokens, query_weight, mixout_weight, lower_bound, recurrent_state.shape[-1]
    ):
        return whole_layer(
            tokens, recurrent_state, query_weight, forget_weight, input_weight, outgate_weight,
            lower_bound, head_gain, mixout_weight, first_gain, first_bias, router_weight,
            branch_vector, dense_gate_weight, dense_up_weight, dense_down_weight,
            expert_gate_weight, expert_up_weight, expert_down_weight, second_gain, second_bias,
            routes,
        )
    nseq, width = tokens.shape
    own_cols = query_weight.shape[1]
    stacked = jnp.concatenate(
        [query_weight.T, forget_weight.T, input_weight.T, outgate_weight.T], axis=0
    )
    owned = project(tokens, stacked, devices, 0)
    projected = (
        owned.reshape(devices, nseq, 4, own_cols)
        .transpose(1, 2, 0, 3)
        .reshape(nseq, 4, devices * own_cols)
    )
    mixed, new_state = recurrence(projected, recurrent_state, lower_bound, head_gain)
    mix_out = project(mixed, mixout_weight.T, devices, 1).transpose(1, 0, 2).reshape(nseq, width)
    normed = layer_norm(
        ALPHA * tokens.astype(f32) + mix_out.astype(f32), first_gain, first_bias
    ).astype(jnp.bfloat16)
    output = channel_and_norm(
        normed,
        routes,
        devices,
        router_weight,
        branch_vector,
        dense_gate_weight,
        dense_up_weight,
        dense_down_weight,
        expert_gate_weight,
        expert_up_weight,
        expert_down_weight,
        second_gain,
        second_bias,
    )
    return (output, new_state)


def solution(mesh):
    return jax.shard_map(
        per_device,
        mesh=mesh,
        in_specs=(
            P("ep", None),
            P("ep", None, None, None),
            P(None, "ep"),
            P(None, "ep"),
            P(None, "ep"),
            P(None, "ep"),
            P(),
            P(),
            P(None, "ep"),
            P(),
            P(),
            P(),
            P(),
            P(None, "ep"),
            P(None, "ep"),
            P("ep", None),
            P(None, "ep"),
            P(None, "ep"),
            P("ep", None),
            P(),
            P(),
            P(),
        ),
        out_specs=(P("ep", None), P("ep", None, None, None)),
        check_vma=False,
    )
```
